32 devices in a mesh: sp: 8 (over z, y), tp: 4 (over x, core).
Axes of the slice: x: 2, y: 2, z: 4, core: 2. Of those that a mesh axis runs over, the one named last changes fastest.
Arguments:
- latent: bfloat16 [4096, 4096], P(('sp', 'tp')), may hold values from -3 to 3
- context: bfloat16 [1024, 4096], P('sp'), may hold values from -6 to 6
- cond: float32 [4096], replicated, may hold values from -6 to 6
- ctx_cond: float32 [4096], replicated, may hold values from -6 to 6
- w_shift: bfloat16 [4096, 4096], P('sp', 'tp'), may hold values from -0.1875 to 0.1875
- w_scale: bfloat16 [4096, 4096], P('sp', 'tp'), may hold values from -0.09375 to 0.15478516
- w_gate: bfloat16 [4096, 4096], P('sp', 'tp'), may hold values from -0.1875 to 0.1875
- w_query: bfloat16 [4096, 2048], P(None, 'tp'), may hold values from -0.09375 to 0.09375
- key_weight: bfloat16 [4096, 1024], P(None, 'tp'), may hold values from -0.09375 to 0.09375
- value_weight: bfloat16 [4096, 1024], P(None, 'tp'), may hold values from -0.09375 to 0.09375
- w_out: bfloat16 [2048, 4096], P('tp'), may hold values from -0.125 to 0.125
- sink: float32 [16], replicated, may hold values from 4 to 8
Outputs:
- mixed: bfloat16 [4096, 4096], P(('sp', 'tp'))
The draws below stay inside these ranges and needn't reach their ends.
All inputs are finite; a program needn't handle non-finite values.
Results may differ from the reference program's by a relative error of at most 0.035.
Values may be sent and summed in bfloat16 or wider, within the bound.
A program may use at most 64 MiB of HBM per device.

```python
import math
import jax
import jax.numpy as jnp
from jax import lax

MODEL_WIDTH = 4096
HEAD_SIZE = 128
QUERY_HEADS = 16
KEY_VALUE_HEADS = 8
WINDOW_SIDE = 128
GRID_WIDTH = 64
CONTEXT_TOKENS = 1024
LATENT_TOKENS = 4096
N_TP = 4


def draw_w_scale(key, part):
    first, second = jax.random.split(jax.random.fold_in(key, 11))
    spread = 2.0 / math.sqrt(MODEL_WIDTH)
    values = jnp.clip(jax.random.normal(first, (MODEL_WIDTH, MODEL_WIDTH), jnp.float32) * spread, -3.0 * spread, 3.0 * spread)
    return values.astype(jnp.bfloat16)


def level_of(stream_key, dims, cuts, least, largest):
    loudness, own = 1.0, jax.random.fold_in(stream_key, 6)
    for dim, shards_of in cuts:
        draws = jnp.exp(jax.random.uniform(jax.random.fold_in(own, dim), (shards_of,), jnp.float32, least / len(cuts), largest / len(cuts)))
        loudness = loudness * jnp.repeat(draws, dims[dim] // shards_of).reshape([-1 if axis == dim else 1 for axis in range(len(dims))])
    return loudness


def normal_values(stream_key, dims, scale, most, shards=(), kind=jnp.bfloat16):
    level = level_of(stream_key, dims, shards, -0.22, 0.18) if shards else 1.0
    values = jax.random.normal(stream_key, dims, jnp.float32) * scale * level
    return jnp.minimum(jnp.maximum(values, -most), most).astype(kind)


def setup_inputs(seed: int = 0) -> dict:
    splits = jax.random.split(jax.random.key(seed), 13)
    return {
        "latent": normal_values(splits[0], (LATENT_TOKENS, MODEL_WIDTH), 0.5, 3.0, ((0, 32),)),
        "context": normal_values(splits[1], (CONTEXT_TOKENS, MODEL_WIDTH), 1.0, 6.0, ((0, 8),)),
        "cond": normal_values(splits[2], (MODEL_WIDTH,), 1.0, 6.0, (), jnp.float32),
        "ctx_cond": normal_values(splits[3], (MODEL_WIDTH,), 1.0, 6.0, (), jnp.float32),
        "w_shift": normal_values(splits[4], (MODEL_WIDTH, MODEL_WIDTH), (MODEL_WIDTH // 4) ** -0.5, 0.1875, ((0, 8), (1, 4))),
        "w_scale": draw_w_scale(jax.random.fold_in(splits[12], 71), 0),
        "w_gate": normal_values(splits[6], (MODEL_WIDTH, MODEL_WIDTH), (MODEL_WIDTH // 4) ** -0.5, 0.1875, ((0, 8), (1, 4))),
        "w_query": normal_values(splits[7], (MODEL_WIDTH, QUERY_HEADS * HEAD_SIZE), MODEL_WIDTH ** -0.5, 0.09375, ((1, 4),)),
        "key_weight": normal_values(splits[8], (MODEL_WIDTH, KEY_VALUE_HEADS * HEAD_SIZE), MODEL_WIDTH ** -0.5, 0.09375, ((1, 4),)),
        "value_weight": normal_values(splits[9], (MODEL_WIDTH, KEY_VALUE_HEADS * HEAD_SIZE), MODEL_WIDTH ** -0.5, 0.09375, ((1, 4),)),
        "w_out": normal_values(splits[10], (QUERY_HEADS * HEAD_SIZE, MODEL_WIDTH), (QUERY_HEADS * HEAD_SIZE) ** -0.5, 0.125, ((0, 4),)),
        "sink": jnp.clip(jax.random.uniform(splits[11], (QUERY_HEADS,), jnp.float32, 4.0, 8.0), 4.0, 8.0),
    }


EPS = 1e-05
THETA = 10000.0
MASKED = -1e+30

def layer_norm(rows):
    values = rows.astype(jnp.float32)
    mean = lax.optimization_barrier(jnp.mean(values, axis=-1, keepdims=True))
    var = lax.optimization_barrier(jnp.mean(jnp.square(values - mean), axis=-1, keepdims=True))
    return (values - mean) * lax.rsqrt(var + EPS)

def rotate_half(values, token_position, width):
    half = width // 2
    inverse = THETA ** (-jnp.arange(half, dtype=jnp.float32) * 2.0 / width)
    angle = token_position.astype(jnp.float32)[:, None] * inverse[None, :]
    cosine = jnp.cos(angle)[:, None, :]
    sine = jnp.sin(angle)[:, None, :]
    first = values[..., :half]
    second = values[..., half:]
    return jnp.concatenate([first * cosine - second * sine, second * cosine + first * sine], axis=-1)

def axial_rotation(heads, token_position, grid):
    width = heads.shape[-1] // 2
    values = heads.astype(jnp.float32)
    turned = jnp.concatenate([rotate_half(values[..., :width], token_position // grid, width), rotate_half(values[..., width:], token_position % grid, width)], axis=-1)
    return turned.astype(jnp.bfloat16)

def sink_weights(scores, sink_column):
    top = jnp.maximum(lax.optimization_barrier(jnp.max(scores, axis=-1, keepdims=True)), sink_column)
    expo = jnp.exp(scores - top)
    return (expo / (lax.optimization_barrier(jnp.sum(expo, axis=-1, keepdims=True)) + jnp.exp(sink_column - top))).astype(jnp.bfloat16)

def reference(latent, context, cond, ctx_cond, w_shift, w_scale, w_gate, w_query, key_weight, value_weight, w_out, sink):
    act = jax.nn.silu(jnp.stack([cond, ctx_cond])).astype(jnp.bfloat16)
    shift = jnp.dot(act, w_shift, preferred_element_type=jnp.float32)
    scale = jnp.dot(act, w_scale, preferred_element_type=jnp.float32)
    gate = jnp.dot(act[0:1], w_gate, preferred_element_type=jnp.float32)[0]
    latent_mod = (layer_norm(latent) * (1.0 + scale[0]) + shift[0]).astype(jnp.bfloat16)
    ctx_mod = (layer_norm(context) * (1.0 + scale[1]) + shift[1]).astype(jnp.bfloat16)
    query_group = QUERY_HEADS // KEY_VALUE_HEADS
    query = jnp.dot(latent_mod, w_query, preferred_element_type=jnp.float32).astype(jnp.bfloat16)
    key = jnp.dot(latent_mod, key_weight, preferred_element_type=jnp.float32).astype(jnp.bfloat16)
    value_rows = jnp.dot(latent_mod, value_weight, preferred_element_type=jnp.float32).astype(jnp.bfloat16)
    context_key_rows = jnp.dot(ctx_mod, key_weight, preferred_element_type=jnp.float32).astype(jnp.bfloat16)
    context_value_rows = jnp.dot(ctx_mod, value_weight, preferred_element_type=jnp.float32).astype(jnp.bfloat16)
    token_position = jnp.arange(LATENT_TOKENS, dtype=jnp.int32)
    rotated_query = axial_rotation(query.reshape(LATENT_TOKENS, QUERY_HEADS, HEAD_SIZE), token_position, GRID_WIDTH)
    rotated_key = axial_rotation(key.reshape(LATENT_TOKENS, KEY_VALUE_HEADS, HEAD_SIZE), token_position, GRID_WIDTH)
    padded_key = jnp.pad(rotated_key, ((WINDOW_SIDE, WINDOW_SIDE), (0, 0), (0, 0)))
    value_padded_rows = jnp.pad(value_rows.reshape(LATENT_TOKENS, KEY_VALUE_HEADS, HEAD_SIZE), ((WINDOW_SIDE, WINDOW_SIDE), (0, 0), (0, 0)))
    context_key_wide = context_key_rows.reshape(CONTEXT_TOKENS, KEY_VALUE_HEADS, HEAD_SIZE).astype(jnp.float32)
    context_value_wide = context_value_rows.reshape(CONTEXT_TOKENS, KEY_VALUE_HEADS, HEAD_SIZE).astype(jnp.float32)
    sink_column = sink.reshape(KEY_VALUE_HEADS, query_group)[:, :, None, None]
    factor = HEAD_SIZE ** (-0.5)
    block_list = LATENT_TOKENS // WINDOW_SIDE
    query_block_list = rotated_query.reshape(block_list, WINDOW_SIDE, KEY_VALUE_HEADS, query_group, HEAD_SIZE)

    def one_block(item):
        qblk, index = item
        start = (index * WINDOW_SIDE).astype(jnp.int32)
        kblk = lax.dynamic_slice_in_dim(padded_key, start, 3 * WINDOW_SIDE, 0).astype(jnp.float32)
        vblk = lax.dynamic_slice_in_dim(value_padded_rows, start, 3 * WINDOW_SIDE, 0).astype(jnp.float32)
        q32 = qblk.astype(jnp.float32)
        band_scores = jnp.einsum('qhgd,khd->hgqk', q32, kblk) * factor
        qpos = start + jnp.arange(WINDOW_SIDE, dtype=jnp.int32)
        kpos = start - WINDOW_SIDE + jnp.arange(3 * WINDOW_SIDE, dtype=jnp.int32)
        valid = (jnp.abs(kpos[None, :] - qpos[:, None]) <= WINDOW_SIDE) & (kpos[None, :] >= 0) & (kpos[None, :] < LATENT_TOKENS)
        band_scores = jnp.where(valid[None, None], band_scores, MASKED)
        ctx_scores = jnp.einsum('qhgd,khd->hgqk', q32, context_key_wide) * factor
        weights = sink_weights(jnp.concatenate([band_scores, ctx_scores], axis=-1), sink_column).astype(jnp.float32)
        out = jnp.einsum('hgqk,khd->qhgd', weights[..., :3 * WINDOW_SIDE], vblk) + jnp.einsum('hgqk,khd->qhgd', weights[..., 3 * WINDOW_SIDE:], context_value_wide)
        return out.astype(jnp.bfloat16).reshape(WINDOW_SIDE, QUERY_HEADS * HEAD_SIZE)
    attended = lax.map(one_block, (query_block_list, jnp.arange(block_list, dtype=jnp.int32))).reshape(LATENT_TOKENS, QUERY_HEADS * HEAD_SIZE)
    columns = QUERY_HEADS * HEAD_SIZE // N_TP
    projected = jnp.zeros((LATENT_TOKENS, MODEL_WIDTH), jnp.float32)
    for group_index in range(N_TP):
        lower = group_index * columns
        partial_product = jnp.dot(attended[:, lower:lower + columns], w_out[lower:lower + columns], preferred_element_type=jnp.float32).astype(jnp.bfloat16)
        projected = projected + partial_product.astype(jnp.float32)
    return (latent.astype(jnp.float32) + gate[None, :] * projected).astype(jnp.bfloat16)
```

```python
import functools
import math

import jax
import jax.numpy as jnp
from jax import lax
from jax.experimental import pallas as pl
from jax.experimental.pallas import tpu as pltpu
from jax.sharding import PartitionSpec as P

HEAD = 128
SIDE = 128
GRID_WIDTH = 64
EPS = 1e-05
THETA = 10000.0
MASKED = -1e30
LOG2E = math.log2(math.e)
MESH = pl.DeviceIdType.MESH
F32 = jnp.float32
BF16 = jnp.bfloat16
TILES = 8
LAG = 3
CORES = 2
FIRST = 16
GROUPS = ((0, 1), (2,), (3,))


def grid_y(nsp):
    ny = math.isqrt(nsp // 2)
    return ny if ny > 0 and nsp % ny == 0 else 1


def body(
    nsp, ntp,
    lat, ctx, cond, ctx_cond, w_shift, w_scale, w_gate, w_q, w_k, w_v, w_o, sink,
    out,
    cos_t, sin_t, st_mean, st_rstd, tslots,
    wmod, wq, wk, wv, wo, latb, ctxb, mb, part, mgath, mod, ctxk, ctxv, q_s, kv, att,
    stage, prcv, comb, xrcv, condb,
    load_sem, msend, mrecv, tsend, trecv, lsend, lrecv, fsend, frecv, psend, precv,
    zsend, zrecv, ysend, yrecv, hsend, hrecv, dsend, drecv, xsend, xrecv,
):
    nx = ntp // CORES
    ny = grid_y(nsp)
    nz = nsp // ny
    sp = lax.axis_index("sp")
    tp = lax.axis_index("tp")
    x = lax.div(tp, CORES)
    c = lax.rem(tp, CORES)
    oc = 1 - c
    z = lax.div(sp, ny)
    y = lax.rem(sp, ny)
    rows, width = lat.shape
    crows = ctx.shape[0]
    tokens = rows * ntp
    mcols = w_shift.shape[1]
    nc = mcols // HEAD
    qc = w_q.shape[1]
    kc = w_k.shape[1]
    kv_heads = kc // HEAD
    group = qc // kc
    edges = [0, FIRST, rows // 2, rows // 4 * 3, rows]
    ncut = len(edges) - 1

    def at_tp(t):
        return (sp, t)

    def at_sp(s):
        return (s, tp)

    partner = at_tp(x * CORES + oc)

    def remote(src, dst, ss, rs, dev):
        return pltpu.make_async_remote_copy(
            src_ref=src, dst_ref=dst, send_sem=ss, recv_sem=rs, device_id=dev, device_id_type=MESH
        )

    loads = [
        pltpu.make_async_copy(s, d, load_sem.at[i])
        for i, (s, d) in enumerate(
            [
                (w_shift, wmod.at[0]), (w_scale, wmod.at[1]), (w_gate, wmod.at[2]),
                (ctx, ctxb), (w_k, wk), (w_v, wv), (w_q, wq),
                (lat, latb.at[tp]), (w_o, wo), (cond, condb.at[0]), (ctx_cond, condb.at[1]),
            ]
        )
    ]
    for i in (9, 10, 0, 1, 2, 7, 3):
        loads[i].start()

    barrier = pltpu.get_barrier_semaphore()
    for d in range(1, nsp):
        pl.semaphore_signal(barrier, inc=1, device_id=at_sp(lax.rem(sp + d, nsp)), device_id_type=MESH)
    for d in range(1, ntp):
        pl.semaphore_signal(barrier, inc=1, device_id=at_tp(lax.rem(tp + d, ntp)), device_id_type=MESH)

    def lat_copy(d, j):
        dst = lax.rem(x + d, nx) * CORES + c
        piece = latb.at[tp, pl.ds(edges[j], edges[j + 1] - edges[j])]
        return remote(piece, piece, lsend.at[d - 1, j], lrecv.at[d - 1, j], at_tp(dst))

    def from_x(d):
        return lax.rem(x - d + nx, nx)

    def fwd_copy(d, j):
        slot = latb.at[from_x(d) * CORES + c, pl.ds(edges[j], edges[j + 1] - edges[j])]
        return remote(slot, slot, fsend.at[d - 1, j], frecv.at[d - 1, j], partner)

    def turn_tables():
        half = HEAD // 2
        lane_i = lax.broadcasted_iota(jnp.int32, (tokens, HEAD), 1)
        inner = lax.rem(lane_i, half // 2).astype(F32)
        inverse = jnp.exp(inner * (-2.0 / half * math.log(THETA)))
        pos = (lax.broadcasted_iota(jnp.int32, (tokens, HEAD), 0) + sp * tokens).astype(F32)
        grid_row = jnp.floor(pos * (1.0 / GRID_WIDTH))
        angle = jnp.where(lane_i < half, grid_row, pos - grid_row * GRID_WIDTH) * inverse
        cos_t[...] = jnp.cos(angle)
        sin_t[...] = jnp.where(lax.rem(lane_i, half) < half // 2, -1.0, 1.0) * jnp.sin(angle)

    turn_tables()
    mrows = w_shift.shape[0]
    arow = pl.ds(pl.multiple_of(sp * mrows, mrows), mrows)
    loads[9].wait()
    loads[10].wait()
    a0 = jax.nn.silu(condb[0:1, arow]).astype(BF16).astype(F32)
    a1 = jax.nn.silu(condb[1:2, arow]).astype(BF16).astype(F32)
    line = lax.broadcasted_iota(jnp.int32, (8, mrows), 0)
    zero = jnp.zeros((8, mrows), F32)
    a0 = jnp.broadcast_to(a0, zero.shape)
    a1 = jnp.broadcast_to(a1, zero.shape)
    acc = None
    for i, (r0, r1) in enumerate(((0, 1), (2, 3), (4, -1))):
        act = jnp.where(line == r0, a0, jnp.where(line == r1, a1, zero)).astype(BF16)
        loads[i].wait()
        piece = jnp.dot(act, wmod[i], preferred_element_type=F32)
        acc = piece if acc is None else acc + piece
    for k, (r0, r1) in enumerate(((1, 3), (0, 2), (4, 4))):
        part[k] = jnp.concatenate(
            [acc[r : r + 1, i * HEAD : (i + 1) * HEAD] for r in (r0, r1) for i in range(nc)], axis=0
        ).astype(BF16)
    pl.semaphore_wait(barrier, nsp + ntp - 2)
    loads[7].wait()
    mcopies = [
        [
            remote(
                part.at[cut], mgath.at[d - 1, cut], msend.at[d - 1, e], mrecv.at[d - 1, e],
                at_sp(lax.rem(sp + d, nsp)),
            )
            for d in range(1, nsp)
        ]
        for e, cut in enumerate((pl.ds(0, 1), pl.ds(1, 2)))
    ]
    for cp in mcopies[0]:
        cp.start()
    for d in range(1, nx):
        lat_copy(d, 0).start()
    for cp in mcopies[1]:
        cp.start()
    own = remote(latb.at[tp], latb.at[tp], psend, precv, partner)
    own.start()
    for i in (4, 5, 6, 8):
        loads[i].start()

    def measure_rows(src, row0, st0, count):
        step = 16

        @pl.loop(0, count // step)
        def _(i):
            v = src[pl.ds(row0 + i * step, step), :]
            parts = [None] * 4
            for j in range(width // HEAD):
                t = v[:, j * HEAD : (j + 1) * HEAD].astype(F32)
                parts[j % 4] = t if parts[j % 4] is None else parts[j % 4] + t
            st_mean[pl.ds(st0 + i * step, step), :] = (parts[0] + parts[1]) + (parts[2] + parts[3])

        whole = pl.ds(st0, count)
        mean = jnp.sum(st_mean[whole, :], axis=-1, keepdims=True) * (1.0 / width)
        st_mean[whole, :] = jnp.broadcast_to(mean, (count, HEAD))

        @pl.loop(0, count // step)
        def _(i):
            v = src[pl.ds(row0 + i * step, step), :]
            m = st_mean[pl.ds(st0 + i * step, step), :]
            parts = [None] * 4
            for j in range(width // HEAD):
                t = v[:, j * HEAD : (j + 1) * HEAD].astype(F32) - m
                t = t * t
                parts[j % 4] = t if parts[j % 4] is None else parts[j % 4] + t
            st_rstd[pl.ds(st0 + i * step, step), :] = (parts[0] + parts[1]) + (parts[2] + parts[3])

        var = jnp.sum(st_rstd[whole, :], axis=-1, keepdims=True) * (1.0 / width)
        st_rstd[whole, :] = jnp.broadcast_to(lax.rsqrt(var + EPS), (count, HEAD))

    def shift_rows(src, row0, st0, dst, dst0, count, r_shift, r_scale):
        step = min(32, count)
        rep = step // 8

        @pl.loop(0, count // step)
        def _(i):
            srow = pl.ds(st0 + i * step, step)
            m = st_mean[srow, :]
            r = st_rstd[srow, :]
            for j in range(width // HEAD):
                cols = slice(j * HEAD, (j + 1) * HEAD)
                v = src[pl.ds(row0 + i * step, step), cols].astype(F32)
                v = (v - m) * r
                sc = jnp.concatenate([mod[r_scale, :, cols]] * rep, axis=0)
                sh = jnp.concatenate([mod[r_shift, :, cols]] * rep, axis=0)
                dst[pl.ds(dst0 + i * step, step), cols] = (v * sc + sh).astype(BF16)

    lat2 = latb.reshape(ntp * rows, width)
    base = pl.multiple_of(x * CORES * rows, CORES * rows)
    measure_rows(lat2, pl.multiple_of(tp * rows, rows), pl.multiple_of(c * rows, rows), rows)
    loads[3].wait()
    measure_rows(ctxb, 0, CORES * rows, crows)
    tcopies = [
        [
            remote(
                tslots.at[tp, cut], tslots.at[tp, cut], tsend.at[d - 1, e], trecv.at[d - 1, e],
                at_tp(lax.rem(tp + d, ntp)),
            )
            for d in range(1, ntp)
        ]
        for e, cut in enumerate((pl.ds(0, 1), pl.ds(1, 2)))
    ]
    for e, cut in enumerate((slice(0, 1), slice(1, 3))):
        acc = part[cut].astype(F32)
        for d in range(1, nsp):
            mcopies[e][d - 1].wait_recv()
            acc = acc + mgath[d - 1, cut].astype(F32)
        tslots[tp, cut] = acc.astype(BF16)
        for cp in tcopies[e]:
            cp.start()
    for d in range(1, nx):
        for j in range(1, ncut):
            lat_copy(d, j).start()
    own.wait_recv()
    measure_rows(lat2, pl.multiple_of((x * CORES + oc) * rows, rows), pl.multiple_of(oc * rows, rows), rows)

    def spread(e, picks):
        for cp in tcopies[e]:
            cp.wait_recv()
        for k, first, r, bump in picks:
            for t in range(ntp):
                v = tslots[t, k].astype(F32)
                for i in range(nc):
                    row = v[first * nc + i : first * nc + i + 1] + bump
                    mod[r, :, t * mcols + i * HEAD : t * mcols + (i + 1) * HEAD] = jnp.broadcast_to(row, (8, HEAD))

    spread(0, ((0, 0, 1, 0.0), (0, 1, 3, 1.0)))
    loads[4].wait()
    loads[5].wait()

    def ctx_block(h, o):
        return (ctxk if h == 0 else ctxv).at[pl.ds(pl.multiple_of(o * crows, crows), crows)]

    def z_copy(way, k, h, o):
        to = jnp.clip(z + (1 if way == 0 else -1), 0, nz - 1) * ny + y
        return remote(ctx_block(h, o), ctx_block(h, o), zsend.at[way, k, h], zrecv.at[way, k, h], at_sp(to))

    def y_copy(d, slot, h, o):
        to = z * ny + lax.rem(y + d, ny)
        return remote(
            ctx_block(h, o), ctx_block(h, o), ysend.at[d - 1, slot, h], yrecv.at[d - 1, slot, h], at_sp(to)
        )

    def arrived(k, way):
        return (z >= k) if way == 0 else (z + k < nz)

    def goes_on(way):
        return (z + 1 < nz) if way == 0 else (z >= 1)

    def origin(k, way):
        return z - k if way == 0 else z + k

    def pass_on(k, way, h, o, act):
        if k < nz - 1:
            @pl.when(goes_on(way))
            def _():
                act(z_copy(way, k, h, o))
        if k > 0 or way == 0:
            for d in range(1, ny):
                act(y_copy(d, 2 * k - 1 + way if k > 0 else 0, h, o))

    def each_block(k, fn):
        for way in range(2):
            if k == 0:
                fn(way, sp)
            else:
                @pl.when(arrived(k, way))
                def _():
                    fn(way, origin(k, way) * ny + y)

    def relay(k, h):
        def one(way, o):
            if k > 0:
                z_copy(way, k - 1, h, o).wait_recv()
            pass_on(k, way, h, o, lambda cp: cp.start())

        each_block(k, one)

    shift_rows(ctxb, 0, CORES * rows, mb, 0, crows, 1, 3)
    crow = pl.ds(pl.multiple_of(sp * crows, crows), crows)
    for h, (w, dst) in enumerate(((wk, ctxk), (wv, ctxv))):
        dst[crow, :] = jnp.dot(mb[0:crows, :], w[...], preferred_element_type=F32).astype(BF16)
        relay(0, h)
    events = [(k, h) for k in range(1, nz) for h in range(2)]

    def poll(n):
        for _ in range(n):
            if events:
                k, h = events.pop(0)
                relay(k, h)

    spread(1, ((1, 0, 0, 0.0), (1, 1, 2, 1.0), (2, 0, 4, 0.0)))

    lane = lax.broadcasted_iota(jnp.int32, (1, HEAD), 1)
    low = lax.rem(lane, HEAD // 2) < HEAD // 4

    def turn(v, row0, count, factor):
        v = v.astype(BF16).astype(F32)
        swapped = jnp.where(low, pltpu.roll(v, HEAD - HEAD // 4, 1), pltpu.roll(v, HEAD // 4, 1))
        r = v * cos_t[pl.ds(row0, count), :] + swapped * sin_t[pl.ds(row0, count), :]
        return (r * factor).astype(BF16)

    def project(segments):
        total = sum(n for _, n in segments)
        qf = HEAD ** (-0.5) * LOG2E
        for w, cols, kind in ((wq, qc, 0), (wk, kc, 1), (wv, kc, 2)):
            tile = min(256, cols)
            for n0 in range(0, cols, tile):
                r = jnp.dot(mb[0:total, :], w[:, n0 : n0 + tile], preferred_element_type=F32)
                off = 0
                for row0, n in segments:
                    for h in range(0, tile, HEAD):
                        v = r[off : off + n, h : h + HEAD]
                        if kind == 0:
                            q_s[pl.ds(row0, n), n0 + h : n0 + h + HEAD] = turn(v, row0, n, qf)
                        elif kind == 1:
                            kv[pl.ds(row0 + SIDE, n), n0 + h : n0 + h + HEAD] = turn(v, row0, n, 1.0)
                        else:
                            kv[pl.ds(row0 + SIDE, n), kc + n0 + h : kc + n0 + h + HEAD] = v.astype(BF16)
                    off += n

    loads[6].wait()
    shift_rows(lat2, base, 0, mb, 0, CORES * rows, 0, 2)
    project([(base, CORES * rows)])
    poll(2)

    left = at_sp(lax.rem(sp + nsp - 1, nsp))
    right = at_sp(lax.rem(sp + 1, nsp))
    to_left = remote(kv.at[pl.ds(SIDE, SIDE)], kv.at[pl.ds(SIDE + tokens, SIDE)], hsend.at[0], hrecv.at[0], left)
    to_right = remote(kv.at[pl.ds(tokens, SIDE)], kv.at[pl.ds(0, SIDE)], hsend.at[1], hrecv.at[1], right)

    for d in range(1, nx):
        for g, cuts in enumerate(GROUPS):
            segments = []
            for j in cuts:
                lat_copy(d, j).wait_recv()
                fwd_copy(d, j).start()
            r0, n = edges[cuts[0]], edges[cuts[-1] + 1] - edges[cuts[0]]
            r_a = pl.multiple_of((from_x(d) * CORES + c) * rows + r0, 16)
            r_b = pl.multiple_of((from_x(d) * CORES + oc) * rows + r0, 16)
            measure_rows(lat2, r_a, 0, n)
            shift_rows(lat2, r_a, 0, mb, 0, n, 0, 2)
            for j in cuts:
                fwd_copy(d, j).wait_recv()
            measure_rows(lat2, r_b, n, n)
            shift_rows(lat2, r_b, n, mb, n, n, 0, 2)
            project([(r_a, n), (r_b, n)])
            if d == 1:
                poll(2)
                if g == 0:
                    @pl.when(x == 0)
                    def _():
                        to_left.start()

                    @pl.when(x == nx - 1)
                    def _():
                        to_right.start()
    poll(len(events))

    @pl.when(x != 0)
    def _():
        to_left.start()

    @pl.when(x != nx - 1)
    def _():
        to_right.start()


    def y_wait(k, way, h):
        for d in range(1, ny):
            o = origin(k, way) * ny + lax.rem(y - d + ny, ny)
            y_copy(d, 2 * k - 1 + way if k > 0 else 0, h, o).wait_recv()

    for h in range(2):
        y_wait(0, 0, h)
    for k in range(1, nz):
        for way in range(2):
            @pl.when(arrived(k, way))
            def _():
                for h in range(2):
                    y_wait(k, way, h)
    loads[8].wait()

    band = rows + 2 * SIDE
    key_i = lax.broadcasted_iota(jnp.int32, (rows, band), 1)
    gap = key_i - lax.broadcasted_iota(jnp.int32, (rows, band), 0)
    near = (gap >= 0) & (gap <= 2 * SIDE)

    def attend(t, u):
        r0 = pl.multiple_of(t * rows, rows)
        kpos = key_i + (sp * tokens + r0 - SIDE)
        valid = near & (kpos >= 0) & (kpos < tokens * nsp)
        bias = jnp.where(valid, 0.0, MASKED)
        bias = jnp.concatenate([bias] * group, axis=0)
        for h in range(kv_heads):
            heads = [h * group + i for i in range(group)]
            q = jnp.concatenate([q_s[pl.ds(r0, rows), j * HEAD : (j + 1) * HEAD] for j in heads], axis=0)
            kb = kv[pl.ds(r0, band), h * HEAD : (h + 1) * HEAD]
            vb = kv[pl.ds(r0, band), kc + h * HEAD : kc + (h + 1) * HEAD]
            kx = ctxk[:, h * HEAD : (h + 1) * HEAD]
            vx = ctxv[:, h * HEAD : (h + 1) * HEAD]
            dims = (((1,), (1,)), ((), ()))
            sb = lax.dot_general(q, kb, dims, preferred_element_type=F32) + bias
            sx = lax.dot_general(q, kx, dims, preferred_element_type=F32)
            snk = jnp.concatenate(
                [jnp.full((rows, 1), sink[tp * (qc // HEAD) + j], F32) for j in heads], axis=0
            ) * LOG2E
            top = jnp.maximum(
                jnp.maximum(jnp.max(sb, axis=-1, keepdims=True), jnp.max(sx, axis=-1, keepdims=True)), snk
            )
            eb = jnp.exp2(sb - top)
            ex = jnp.exp2(sx - top)
            den = jnp.sum(eb, axis=-1, keepdims=True) + jnp.sum(ex, axis=-1, keepdims=True) + jnp.exp2(snk - top)
            o = jnp.dot(eb.astype(BF16), vb, preferred_element_type=F32) + jnp.dot(
                ex.astype(BF16), vx, preferred_element_type=F32
            )
            o = (o / den).astype(BF16)
            for i, j in enumerate(heads):
                att[pl.ds(pl.multiple_of(u * rows, rows), rows), j * HEAD : (j + 1) * HEAD] = o[i * rows : (i + 1) * rows]

    tile_cols = width // TILES

    def cols_of(n):
        return slice(n * tile_cols, (n + 1) * tile_cols)

    def x_copy(g, n, xo):
        return remote(
            comb.at[g, n], xrcv.at[g, n], xsend.at[g, n], xrecv.at[g, n], at_tp(xo * CORES + c)
        )

    def d_copy(g, n):
        return remote(stage.at[g, n, pl.ds(0, rows)], prcv.at[g, n], dsend.at[g, n], drecv.at[g, n], partner)

    def combine(g, n, xo):
        d_copy(g, n).wait_recv()
        if g < nx - 1:
            comb[g, n] = (stage[g, n, rows : 2 * rows].astype(F32) + prcv[g, n].astype(F32)).astype(BF16)
            x_copy(g, n, xo).start()

    for g in range(nx):
        xo = lax.rem(x + 1 + g, nx)
        if g == 0:
            @pl.when(x != 0)
            def _():
                to_right.wait_recv()

            @pl.when(x != nx - 1)
            def _():
                to_left.wait_recv()
        if g == nx - 1:
            @pl.when(x == 0)
            def _():
                to_right.wait_recv()

            @pl.when(x == nx - 1)
            def _():
                to_left.wait_recv()


        @pl.loop(0, 2)
        def _(u):
            attend(xo * CORES + lax.rem(oc + u, 2), u)

        for n in range(TILES + LAG):
            if n < TILES:
                stage[g, n] = jnp.dot(att[...], wo[:, cols_of(n)], preferred_element_type=F32).astype(BF16)
                d_copy(g, n).start()
            if n >= LAG:
                combine(g, n - LAG, xo)

    last = nx - 1
    for n in range(TILES):
        total = stage[last, n, rows : 2 * rows].astype(F32) + prcv[last, n].astype(F32)
        for g in range(nx - 1):
            x_copy(g, n, lax.rem(x + 1 + g, nx)).wait_recv()
            total = total + xrcv[g, n].astype(F32)
        out[:, cols_of(n)] = (latb[tp, :, cols_of(n)].astype(F32) + mod[4, 0:1, cols_of(n)] * total).astype(BF16)

    for cp in mcopies[0] + mcopies[1] + tcopies[0] + tcopies[1] + [own, to_left, to_right]:
        cp.wait_send()
    for k in range(nz):
        for h in range(2):
            each_block(k, lambda way, o, k=k, h=h: pass_on(k, way, h, o, lambda cp: cp.wait_send()))
    for d in range(1, nx):
        for j in range(ncut):
            lat_copy(d, j).wait_send()
            fwd_copy(d, j).wait_send()
    for g in range(nx):
        for n in range(TILES):
            d_copy(g, n).wait_send()
            if g < nx - 1:
                x_copy(g, n, lax.rem(x + 1 + g, nx)).wait_send()


def shards(lat, ctx, cond, ctx_cond, w_shift, w_scale, w_gate, w_q, w_k, w_v, w_o, sink):
    nsp = lax.axis_size("sp")
    ntp = lax.axis_size("tp")
    nx = ntp // CORES
    ny = grid_y(nsp)
    nz = nsp // ny
    hops = max(nz - 1, 1)
    rows, width = lat.shape
    crows = ctx.shape[0]
    tokens = rows * ntp
    qc = w_q.shape[1]
    kc = w_k.shape[1]
    mrows, mcols = w_shift.shape
    nc2 = 2 * (mcols // HEAD)
    ncut = 4
    any_ = pl.BlockSpec(memory_space=pl.ANY)
    vmem = pl.BlockSpec(memory_space=pltpu.VMEM)
    dma = pltpu.SemaphoreType.DMA
    V = pltpu.VMEM
    return pl.pallas_call(
        functools.partial(body, nsp, ntp),
        out_shape=pltpu.VMEM((rows, width), BF16),
        in_specs=[any_] * 11 + [pl.BlockSpec(memory_space=pltpu.SMEM)],
        out_specs=vmem,
        scratch_shapes=[
            V((tokens, HEAD), F32), V((tokens, HEAD), F32), V((CORES * rows + crows, HEAD), F32),
            V((CORES * rows + crows, HEAD), F32), V((ntp, 3, nc2, HEAD), BF16),
            V((3, mrows, mcols), BF16), V((width, qc), BF16), V((width, kc), BF16), V((width, kc), BF16),
            V((qc, width), BF16), V((ntp, rows, width), BF16), V((crows, width), BF16),
            V((max(CORES * rows, crows), width), BF16), V((3, nc2, HEAD), BF16), V((nsp - 1, 3, nc2, HEAD), BF16),
            V((5, 8, width), F32), V((nsp * crows, kc), BF16), V((nsp * crows, kc), BF16), V((tokens, qc), BF16),
            V((tokens + 2 * SIDE, 2 * kc), BF16), V((2 * rows, qc), BF16),
            V((nx, TILES, 2 * rows, width // TILES), BF16), V((nx, TILES, rows, width // TILES), BF16),
            V((nx - 1, TILES, rows, width // TILES), BF16), V((nx - 1, TILES, rows, width // TILES), BF16),
            V((2, width), F32),
            dma((11,)), dma((nsp - 1, 2)), dma((nsp - 1, 2)), dma((ntp - 1, 2)), dma((ntp - 1, 2)),
            dma((nx - 1, ncut)), dma((nx - 1, ncut)), dma((nx - 1, ncut)), dma((nx - 1, ncut)), dma, dma,
            dma((2, hops, 2)), dma((2, hops, 2)), dma((max(ny - 1, 1), 2 * nz - 1, 2)),
            dma((max(ny - 1, 1), 2 * nz - 1, 2)), dma((2,)), dma((2,)), dma((nx, TILES)), dma((nx, TILES)),
            dma((nx - 1, TILES)), dma((nx - 1, TILES)),
        ],
        compiler_params=pltpu.CompilerParams(
            collective_id=0, has_side_effects=True, vmem_limit_bytes=60 * 1024 * 1024
        ),
    )(
        lat, ctx, cond, ctx_cond,
        w_shift, w_scale, w_gate, w_q, w_k, w_v, w_o, sink,
    )


def solution(mesh):
    in_specs = (
        P(("sp", "tp"), None), P("sp", None), P(), P(), P("sp", "tp"), P("sp", "tp"), P("sp", "tp"),
        P(None, "tp"), P(None, "tp"), P(None, "tp"), P("tp", None), P(),
    )
    return jax.shard_map(
        shards, mesh=mesh, in_specs=in_specs, out_specs=P(("sp", "tp"), None), check_vma=False
    )
```

```python
import functools
import math

import jax
import jax.numpy as jnp
from jax import lax
from jax.experimental import pallas as pl
from jax.experimental.pallas import tpu as pltpu
from jax.sharding import PartitionSpec as P

HEAD = 128
SIDE = 128
GRID_WIDTH = 64
EPS = 1e-05
THETA = 10000.0
MASKED = -1e30
LOG2E = math.log2(math.e)
MESH = pl.DeviceIdType.MESH
F32 = jnp.float32
BF16 = jnp.bfloat16
UNIT = 16
TILES = 4
CORES = 2


def grid_y(nsp):
    ny = math.isqrt(nsp // 2)
    return ny if ny > 0 and nsp % ny == 0 else 1


def unit_plan(rows):
    units = rows // UNIT
    rest = [u for u in range(2 * units) if u % units]
    steps = [(0, units)] + list(zip(rest[0::2], rest[1::2]))
    fresh, used = [], 0
    for quarter in range(1, 5):
        need = 1 + max(i for i, pair in enumerate(steps) if min(pair) < quarter * units // 2)
        fresh.append(list(range(used, max(need, used))))
        used = max(need, used)
    return units, steps, fresh


def body(
    nsp, ntp,
    lat, ctx, cond, ctx_cond, w_shift, w_scale, w_gate, w_q, w_k, w_v, w_o, sink_h,
    out,
    cos_t, sin_t, st_mean, st_rstd, tslots,
    wmod, wq, wk, wv, wo, latb, ctxb, mb, part, mgath, mod, ctxk, ctxv, q_s, kv, att,
    away, keep, prcv, comb, xrcv, stage, orcv, condb, sink,
    load_sem, msend, mrecv, tsend, trecv, lsend, lrecv, fsend, frecv, psend, precv,
    zsend, zrecv, ysend, yrecv, hsend, hrecv, dsend, drecv, xsend, xrecv, osend, orecv,
):
    nx = ntp // CORES
    ny = grid_y(nsp)
    nz = nsp // ny
    sp = lax.axis_index("sp")
    tp = lax.axis_index("tp")
    x = lax.div(tp, CORES)
    c = lax.rem(tp, CORES)
    oc = 1 - c
    z = lax.div(sp, ny)
    y = lax.rem(sp, ny)
    rows, width = lat.shape
    crows = ctx.shape[0]
    tokens = rows * ntp
    mcols = w_shift.shape[1]
    nc = mcols // HEAD
    qc = w_q.shape[1]
    kc = w_k.shape[1]
    kv_heads = kc // HEAD
    group = qc // kc
    chip = CORES * rows
    units, steps, fresh = unit_plan(rows)

    def at_tp(t):
        return (sp, t)

    def at_sp(s):
        return (s, tp)

    partner = at_tp(x * CORES + oc)

    def remote(src, dst, ss, rs, dev):
        return pltpu.make_async_remote_copy(
            src_ref=src, dst_ref=dst, send_sem=ss, recv_sem=rs, device_id=dev, device_id_type=MESH
        )

    mine = pl.ds(pl.multiple_of(tp * rows, rows), rows)
    loads = [
        pltpu.make_async_copy(s, d, load_sem.at[i])
        for i, (s, d) in enumerate(
            [
                (w_shift, wmod.at[0]), (w_scale, wmod.at[1]), (w_gate, wmod.at[2]),
                (ctx, ctxb), (w_k, wk), (w_v, wv), (w_q, wq),
                (lat, latb.at[mine]), (w_o, wo), (cond, condb.at[0]), (ctx_cond, condb.at[1]), (sink_h, sink),
            ]
        )
    ]
    for i in (9, 10, 0, 1, 2, 7, 3, 11):
        loads[i].start()

    barrier = pltpu.get_barrier_semaphore()
    for d in range(1, nsp):
        pl.semaphore_signal(barrier, inc=1, device_id=at_sp(lax.rem(sp + d, nsp)), device_id_type=MESH)
    for d in range(1, ntp):
        pl.semaphore_signal(barrier, inc=1, device_id=at_tp(lax.rem(tp + d, ntp)), device_id_type=MESH)

    def from_x(d):
        return lax.rem(x - d + nx, nx)

    def chip_rows(xc, k, core):
        first, second = steps[k]
        start = xc * chip + (first + core * (second - first)) * UNIT
        return latb.at[pl.ds(pl.multiple_of(start, UNIT), UNIT)]

    def lat_copy(d, k, xc):
        dst = lax.rem(x + d, nx) * CORES + c
        return remote(chip_rows(xc, k, c), chip_rows(xc, k, c), lsend.at[d - 1], lrecv.at[d - 1, k], at_tp(dst))

    def fwd_copy(d, k, core):
        piece = chip_rows(from_x(d), k, core)
        return remote(piece, piece, fsend.at[d - 1], frecv.at[d - 1, k], partner)

    def turn_tables():
        half = HEAD // 2
        lane_i = lax.broadcasted_iota(jnp.int32, (tokens, HEAD), 1)
        inner = lax.rem(lane_i, half // 2).astype(F32)
        inverse = jnp.exp(inner * (-2.0 / half * math.log(THETA)))
        pos = (lax.broadcasted_iota(jnp.int32, (tokens, HEAD), 0) + sp * tokens).astype(F32)
        grid_row = jnp.floor(pos * (1.0 / GRID_WIDTH))
        angle = jnp.where(lane_i < half, grid_row, pos - grid_row * GRID_WIDTH) * inverse
        cos_t[...] = jnp.cos(angle)
        sin_t[...] = jnp.where(lax.rem(lane_i, half) < half // 2, -1.0, 1.0) * jnp.sin(angle)

    turn_tables()
    mrows = w_shift.shape[0]
    arow = pl.ds(pl.multiple_of(sp * mrows, mrows), mrows)
    loads[9].wait()
    loads[10].wait()
    a0 = jax.nn.silu(condb[0:1, arow]).astype(BF16).astype(F32)
    a1 = jax.nn.silu(condb[1:2, arow]).astype(BF16).astype(F32)
    line = lax.broadcasted_iota(jnp.int32, (8, mrows), 0)
    zero = jnp.zeros((8, mrows), F32)
    a0 = jnp.broadcast_to(a0, zero.shape)
    a1 = jnp.broadcast_to(a1, zero.shape)
    acc = None
    for i, (r0, r1) in enumerate(((0, 1), (2, 3), (4, -1))):
        act = jnp.where(line == r0, a0, jnp.where(line == r1, a1, zero)).astype(BF16)
        loads[i].wait()
        piece = jnp.dot(act, wmod[i], preferred_element_type=F32)
        acc = piece if acc is None else acc + piece
    for k, (r0, r1) in enumerate(((1, 3), (0, 2), (4, 4))):
        part[k] = jnp.concatenate(
            [acc[r : r + 1, i * HEAD : (i + 1) * HEAD] for r in (r0, r1) for i in range(nc)], axis=0
        ).astype(BF16)
    pl.semaphore_wait(barrier, nsp + ntp - 2)
    loads[7].wait()
    mcopies = [
        [
            remote(
                part.at[cut], mgath.at[d - 1, cut], msend, mrecv.at[e],
                at_sp(lax.rem(sp + d, nsp)),
            )
            for d in range(1, nsp)
        ]
        for e, cut in enumerate((pl.ds(0, 1), pl.ds(1, 2)))
    ]
    for cp in mcopies[0]:
        cp.start()
    for d in range(1, nx):
        lat_copy(d, 0, x).start()
    for cp in mcopies[1]:
        cp.start()
    own = remote(latb.at[mine], latb.at[mine], psend, precv, partner)
    own.start()
    for i in (4, 5, 6, 8):
        loads[i].start()

    def measure_rows(src, row0, st0, count):
        step = 16

        @pl.loop(0, count // step)
        def _(i):
            v = src[pl.ds(row0 + i * step, step), :]
            parts = [None] * 4
            for j in range(width // HEAD):
                t = v[:, j * HEAD : (j + 1) * HEAD].astype(F32)
                parts[j % 4] = t if parts[j % 4] is None else parts[j % 4] + t
            st_mean[pl.ds(st0 + i * step, step), :] = (parts[0] + parts[1]) + (parts[2] + parts[3])

        whole = pl.ds(st0, count)
        mean = jnp.sum(st_mean[whole, :], axis=-1, keepdims=True) * (1.0 / width)
        st_mean[whole, :] = jnp.broadcast_to(mean, (count, HEAD))

        @pl.loop(0, count // step)
        def _(i):
            v = src[pl.ds(row0 + i * step, step), :]
            m = st_mean[pl.ds(st0 + i * step, step), :]
            parts = [None] * 4
            for j in range(width // HEAD):
                t = v[:, j * HEAD : (j + 1) * HEAD].astype(F32) - m
                t = t * t
                parts[j % 4] = t if parts[j % 4] is None else parts[j % 4] + t
            st_rstd[pl.ds(st0 + i * step, step), :] = (parts[0] + parts[1]) + (parts[2] + parts[3])

        var = jnp.sum(st_rstd[whole, :], axis=-1, keepdims=True) * (1.0 / width)
        st_rstd[whole, :] = jnp.broadcast_to(lax.rsqrt(var + EPS), (count, HEAD))

    def shift_rows(src, row0, st0, dst, dst0, count, r_shift, r_scale):
        step = min(32, count)
        rep = step // 8

        @pl.loop(0, count // step)
        def _(i):
            srow = pl.ds(st0 + i * step, step)
            m = st_mean[srow, :]
            r = st_rstd[srow, :]
            for j in range(width // HEAD):
                cols = slice(j * HEAD, (j + 1) * HEAD)
                v = src[pl.ds(row0 + i * step, step), cols].astype(F32)
                v = (v - m) * r
                sc = jnp.concatenate([mod[r_scale, :, cols]] * rep, axis=0)
                sh = jnp.concatenate([mod[r_shift, :, cols]] * rep, axis=0)
                dst[pl.ds(dst0 + i * step, step), cols] = (v * sc + sh).astype(BF16)

    base = pl.multiple_of(x * chip, chip)
    measure_rows(latb, pl.multiple_of(tp * rows, rows), pl.multiple_of(c * rows, rows), rows)
    loads[3].wait()
    measure_rows(ctxb, 0, chip, crows)
    tcopies = [
        [
            remote(
                tslots.at[tp, cut], tslots.at[tp, cut], tsend, trecv.at[e],
                at_tp(lax.rem(tp + d, ntp)),
            )
            for d in range(1, ntp)
        ]
        for e, cut in enumerate((pl.ds(0, 1), pl.ds(1, 2)))
    ]
    for e, cut in enumerate((slice(0, 1), slice(1, 3))):
        acc = part[cut].astype(F32)
        arrivals = mgath.at[:, cut]
        remote(arrivals, arrivals, msend, mrecv.at[e], partner).wait_recv()
        for d in range(1, nsp):
            acc = acc + mgath[d - 1, cut].astype(F32)
        tslots[tp, cut] = acc.astype(BF16)
        for cp in tcopies[e]:
            cp.start()
        if e == 0:
            own.wait_recv()
        for d in range(1, nx):
            for k in (1,) if e == 0 else range(2, len(steps)):
                lat_copy(d, k, x).start()
    measure_rows(latb, pl.multiple_of((x * CORES + oc) * rows, rows), pl.multiple_of(oc * rows, rows), rows)

    def spread(e, picks):
        others = tslots.at[pl.ds(0, ntp - 1), slice(0, 1) if e == 0 else slice(1, 3)]
        remote(others, others, tsend, trecv.at[e], partner).wait_recv()
        for k, first, r, bump in picks:
            for t in range(ntp):
                v = tslots[t, k].astype(F32)
                for i in range(nc):
                    row = v[first * nc + i : first * nc + i + 1] + bump
                    mod[r, :, t * mcols + i * HEAD : t * mcols + (i + 1) * HEAD] = jnp.broadcast_to(row, (8, HEAD))

    spread(0, ((0, 0, 1, 0.0), (0, 1, 3, 1.0)))
    loads[4].wait()
    loads[5].wait()

    def ctx_block(h, o):
        return (ctxk if h == 0 else ctxv).at[pl.ds(pl.multiple_of(o * crows, crows), crows)]

    def z_copy(way, k, h, o):
        to = jnp.clip(z + (1 if way == 0 else -1), 0, nz - 1) * ny + y
        return remote(ctx_block(h, o), ctx_block(h, o), zsend.at[way, k], zrecv.at[way, k, h], at_sp(to))

    def y_copy(d, h, o):
        to = z * ny + lax.rem(y + d, ny)
        return remote(
            ctx_block(h, o), ctx_block(h, o), ysend.at[d - 1, h], yrecv.at[d - 1, h], at_sp(to)
        )

    def arrived(k, way):
        return (z >= k) if way == 0 else (z + k < nz)

    def goes_on(way):
        return (z + 1 < nz) if way == 0 else (z >= 1)

    def origin(k, way):
        return z - k if way == 0 else z + k

    def pass_on(k, way, h, o, act):
        if k < nz - 1:
            @pl.when(goes_on(way))
            def _():
                act(z_copy(way, k, h, o))
        if k > 0 or way == 0:
            for d in range(1, ny):
                act(y_copy(d, h, o))

    def each_block(k, fn):
        for way in range(2):
            if k == 0:
                fn(way, sp)
            else:
                @pl.when(arrived(k, way))
                def _():
                    fn(way, origin(k, way) * ny + y)

    def relay(k, h):
        def one(way, o):
            if k > 0:
                z_copy(way, k - 1, h, o).wait_recv()
            pass_on(k, way, h, o, lambda cp: cp.start())

        each_block(k, one)

    shift_rows(ctxb, 0, chip, mb, 0, crows, 1, 3)
    crow = pl.ds(pl.multiple_of(sp * crows, crows), crows)
    for w, dst in ((wk, ctxk), (wv, ctxv)):
        dst[crow, :] = jnp.dot(mb[0:crows, :], w[...], preferred_element_type=F32).astype(BF16)
    for h in range(2):
        relay(0, h)
    events = [(k, h) for k in range(1, nz) for h in range(2)]

    def poll(n):
        for _ in range(n):
            if events:
                k, h = events.pop(0)
                relay(k, h)

    spread(1, ((1, 0, 0, 0.0), (1, 1, 2, 1.0), (2, 0, 4, 0.0)))

    lane = lax.broadcasted_iota(jnp.int32, (1, HEAD), 1)
    low = lax.rem(lane, HEAD // 2) < HEAD // 4

    def turn(v, row0, count, factor):
        v = v.astype(BF16).astype(F32)
        swapped = jnp.where(low, pltpu.roll(v, HEAD - HEAD // 4, 1), pltpu.roll(v, HEAD // 4, 1))
        r = v * cos_t[pl.ds(row0, count), :] + swapped * sin_t[pl.ds(row0, count), :]
        return (r * factor).astype(BF16)

    def project(segments):
        total = sum(n for _, n in segments)
        qf = HEAD ** (-0.5) * LOG2E
        for w, cols, kind in ((wq, qc, 0), (wk, kc, 1), (wv, kc, 2)):
            tile = min(256, cols)
            for n0 in range(0, cols, tile):
                r = jnp.dot(mb[0:total, :], w[:, n0 : n0 + tile], preferred_element_type=F32)
                off = 0
                for row0, n in segments:
                    for h in range(0, tile, HEAD):
                        v = r[off : off + n, h : h + HEAD]
                        if kind == 0:
                            q_s[pl.ds(row0, n), n0 + h : n0 + h + HEAD] = turn(v, row0, n, qf)
                        elif kind == 1:
                            kv[pl.ds(row0 + SIDE, n), n0 + h : n0 + h + HEAD] = turn(v, row0, n, 1.0)
                        else:
                            kv[pl.ds(row0 + SIDE, n), kc + n0 + h : kc + n0 + h + HEAD] = v.astype(BF16)
                    off += n

    loads[6].wait()
    shift_rows(latb, base, 0, mb, 0, chip, 0, 2)
    project([(base, chip)])
    left = at_sp(lax.rem(sp + nsp - 1, nsp))
    right = at_sp(lax.rem(sp + 1, nsp))
    to_left = remote(kv.at[pl.ds(SIDE, SIDE)], kv.at[pl.ds(SIDE + tokens, SIDE)], hsend, hrecv.at[0], left)
    to_right = remote(kv.at[pl.ds(tokens, SIDE)], kv.at[pl.ds(0, SIDE)], hsend, hrecv.at[1], right)

    def gather(d, quarter):
        for i, k in enumerate(fresh[quarter]):
            lat_copy(d, k, from_x(d)).wait_recv()
            fwd_copy(d, k, c).start()
            if i == 0 and d == 1:
                poll(2)

    def normalize(d, quarter, dst0):
        for k in fresh[quarter]:
            fwd_copy(d, k, oc).wait_recv()
        n = units // 2 * UNIT
        row0 = pl.multiple_of(from_x(d) * chip + quarter * n, n)
        measure_rows(latb, row0, dst0, n)
        shift_rows(latb, row0, dst0, mb, dst0, n, 0, 2)

    def project_chip(d, quarter, count):
        n = units // 2 * UNIT
        project([(pl.multiple_of(from_x(d) * chip + quarter * n, n), count * n)])

    def wait_context():
        poll(len(events))
        for d in range(1, ny):
            for h, ref in enumerate((ctxk, ctxv)):
                column = ref.at[pl.ds(0, nz * crows)]
                remote(column, column, ysend.at[d - 1, h], yrecv.at[d - 1, h], partner).wait_recv()

    def attend(r0, n, dst0):
        band = n + 2 * SIDE
        key_i = lax.broadcasted_iota(jnp.int32, (n, band), 1)
        gap = key_i - lax.broadcasted_iota(jnp.int32, (n, band), 0)
        kpos = key_i + (sp * tokens + r0 - SIDE)
        valid = (gap >= 0) & (gap <= 2 * SIDE) & (kpos >= 0) & (kpos < tokens * nsp)
        bias = jnp.where(valid, 0.0, MASKED)
        bias = jnp.concatenate([bias] * group, axis=0)
        for h in range(kv_heads):
            heads = [h * group + i for i in range(group)]
            q = jnp.concatenate([q_s[pl.ds(r0, n), j * HEAD : (j + 1) * HEAD] for j in heads], axis=0)
            kb = kv[pl.ds(r0, band), h * HEAD : (h + 1) * HEAD]
            vb = kv[pl.ds(r0, band), kc + h * HEAD : kc + (h + 1) * HEAD]
            kx = ctxk[:, h * HEAD : (h + 1) * HEAD]
            vx = ctxv[:, h * HEAD : (h + 1) * HEAD]
            dims = (((1,), (1,)), ((), ()))
            sb = lax.dot_general(q, kb, dims, preferred_element_type=F32) + bias
            sx = lax.dot_general(q, kx, dims, preferred_element_type=F32)
            snk = jnp.concatenate(
                [jnp.full((n, 1), sink[tp * (qc // HEAD) + j], F32) for j in heads], axis=0
            ) * LOG2E
            top = jnp.maximum(
                jnp.maximum(jnp.max(sb, axis=-1, keepdims=True), jnp.max(sx, axis=-1, keepdims=True)), snk
            )
            eb = jnp.exp2(sb - top)
            ex = jnp.exp2(sx - top)
            den = jnp.sum(eb, axis=-1, keepdims=True) + jnp.sum(ex, axis=-1, keepdims=True) + jnp.exp2(snk - top)
            o = jnp.dot(eb.astype(BF16), vb, preferred_element_type=F32) + jnp.dot(
                ex.astype(BF16), vx, preferred_element_type=F32
            )
            o = (o / den).astype(BF16)
            for i, j in enumerate(heads):
                att[pl.ds(dst0, n), j * HEAD : (j + 1) * HEAD] = o[i * n : (i + 1) * n]

    tile_cols = width // TILES
    half = TILES // CORES
    jobs = ((0, rows // 2, 0), (rows // 2, rows, 0), (rows, chip, 1))

    def cols_of(n):
        return slice(n * tile_cols, (n + 1) * tile_cols)

    def dyn_cols(n):
        return pl.ds(pl.multiple_of(n * tile_cols, tile_cols), tile_cols)

    def d_copy(g, j, i):
        a, b, _ = jobs[j]
        span = pl.ds(a, b - a)
        return remote(away.at[g, i, span], prcv.at[g, i, span], dsend, drecv.at[g, j, i], partner)

    def x_copy(g, j, i, sender):
        a, b, owner = jobs[j]
        xo = lax.rem(x + 1 + g, nx)
        return remote(
            comb.at[g, i, pl.ds(a, b - a)], xrcv.at[g, sender * half + i, pl.ds(a - owner * rows, b - a)],
            xsend, xrecv.at[g, j - owner * 2, sender * half + i], at_tp(xo * CORES + owner),
        )

    def chip_job(g, j):
        a, b, _ = jobs[j]
        xo = lax.rem(x + 1 + g, nx)
        attend(pl.multiple_of(xo * chip + a, UNIT), b - a, a)
        for ref, core in ((away, oc), (keep, c)):
            for i in range(half):
                ref[g, i, a:b] = jnp.dot(
                    att[a:b, :], wo[:, dyn_cols(core * half + i)], preferred_element_type=F32
                ).astype(BF16)
                if ref is away:
                    d_copy(g, j, i).start()

    def combine(g, j):
        a, b, _ = jobs[j]
        for i in range(half):
            d_copy(g, j, i).wait_recv()
            comb[g, i, a:b] = (keep[g, i, a:b].astype(F32) + prcv[g, i, a:b].astype(F32)).astype(BF16)
            x_copy(g, j, i, c).start()

    def halo(first):
        @pl.when((x == 0) if first else (x != 0))
        def _():
            to_left.start()

        @pl.when((x == nx - 1) if first else (x != nx - 1))
        def _():
            to_right.start()

    def wait_halo(first):

        @pl.when((x != 0) if first else (x == 0))
        def _():
            to_right.wait_recv()

        @pl.when((x != nx - 1) if first else (x == nx - 1))
        def _():
            to_left.wait_recv()

    for d in range(1, nx):
        for quarter in range(4):
            gather(d, quarter)
            if quarter == 3 and nx == 2:
                combine(0, 0)
            normalize(d, quarter, quarter * (units // 2 * UNIT) if quarter < 2 else 0)
            if quarter > 0:
                project_chip(d, max(quarter - 1, 0) if quarter == 1 else quarter, 2 if quarter == 1 else 1)
            if quarter == 1 and d == 1:
                halo(True)
            if quarter == 2 and nx == 2:
                wait_context()
                wait_halo(True)
                loads[8].wait()
                loads[11].wait()
                chip_job(0, 0)
    halo(False)
    if nx > 2:
        wait_context()
        wait_halo(True)
        loads[8].wait()
        loads[11].wait()
    for g in range(nx - 1):
        for j in range(1 if nx == 2 else 0, len(jobs)):
            chip_job(g, j)
            combine(g, j)
    wait_halo(False)

    @pl.loop(0, 2)
    def _(u):
        attend(
            pl.multiple_of(base + lax.rem(oc + u, 2) * rows, rows), rows, pl.multiple_of(u * rows, rows)
        )

    own_copy = remote(stage.at[:, pl.ds(0, rows)], orcv, osend, orecv, partner)
    for n in range(TILES):
        stage[n] = jnp.dot(att[...], wo[:, cols_of(n)], preferred_element_type=F32).astype(BF16)
    own_copy.start()
    own_copy.wait_recv()

    def finish(j):
        a, b, owner = jobs[j]
        span = slice(a - owner * rows, b - owner * rows)
        for i in range(half):
            for sender in range(CORES):
                n = sender * half + i
                part_rows = slice(rows + span.start, rows + span.stop)
                total = stage[n, part_rows].astype(F32) + orcv[n, span].astype(F32)
                for g in range(nx - 1):
                    x_copy(g, j, i, sender).wait_recv()
                    total = total + xrcv[g, n, span].astype(F32)
                rows_of = pl.ds(pl.multiple_of(tp * rows, rows) + span.start, b - a)
                out[span, cols_of(n)] = (
                    latb[rows_of, cols_of(n)].astype(F32) + mod[4, 0:1, cols_of(n)] * total
                ).astype(BF16)

    for owner in range(CORES):
        @pl.when(c == owner)
        def _():
            for j in range(len(jobs)):
                if jobs[j][2] == owner:
                    finish(j)


    def sent(ref, sem):
        remote(ref, ref, sem, sem, partner).wait_send()

    own.wait_send()
    own_copy.wait_send()
    sent(mgath, msend)
    sent(tslots.at[pl.ds(0, ntp - 1)], tsend)
    sent(kv.at[pl.ds(0, 2 * SIDE)], hsend)
    for k in range(nz - 1):
        for way in range(2):
            @pl.when(goes_on(way) & (arrived(k, way) if k > 0 else True))
            def _():
                sent(ctxk.at[pl.ds(0, 2 * crows)], zsend.at[way, k])
    for d in range(1, ny):
        for h in range(2):
            sent(ctxk.at[pl.ds(0, nz * crows)], ysend.at[d - 1, h])
    for d in range(1, nx):
        sent(latb.at[pl.ds(0, rows)], lsend.at[d - 1])
        sent(latb.at[pl.ds(0, rows)], fsend.at[d - 1])
    sent(prcv, dsend)
    sent(comb, xsend)


def shards(lat, ctx, cond, ctx_cond, w_shift, w_scale, w_gate, w_q, w_k, w_v, w_o, sink):
    nsp = lax.axis_size("sp")
    ntp = lax.axis_size("tp")
    nx = ntp // CORES
    ny = grid_y(nsp)
    nz = nsp // ny
    hops = max(nz - 1, 1)
    rows, width = lat.shape
    crows = ctx.shape[0]
    tokens = rows * ntp
    qc = w_q.shape[1]
    kc = w_k.shape[1]
    mrows, mcols = w_shift.shape
    nc2 = 2 * (mcols // HEAD)
    _, steps, _ = unit_plan(rows)
    half = TILES // CORES
    any_ = pl.BlockSpec(memory_space=pl.ANY)
    vmem = pl.BlockSpec(memory_space=pltpu.VMEM)
    dma = pltpu.SemaphoreType.DMA
    V = pltpu.VMEM
    return pl.pallas_call(
        functools.partial(body, nsp, ntp),
        out_shape=pltpu.VMEM((rows, width), BF16),
        in_specs=[any_] * 12,
        out_specs=vmem,
        scratch_shapes=[
            V((tokens, HEAD), F32), V((tokens, HEAD), F32), V((CORES * rows + crows, HEAD), F32),
            V((CORES * rows + crows, HEAD), F32), V((ntp, 3, nc2, HEAD), BF16),
            V((3, mrows, mcols), BF16), V((width, qc), BF16), V((width, kc), BF16), V((width, kc), BF16),
            V((qc, width), BF16), V((ntp * rows, width), BF16), V((crows, width), BF16),
            V((max(CORES * rows, crows), width), BF16), V((3, nc2, HEAD), BF16), V((nsp - 1, 3, nc2, HEAD), BF16),
            V((5, 8, width), F32), V((nsp * crows, kc), BF16), V((nsp * crows, kc), BF16), V((tokens, qc), BF16),
            V((tokens + 2 * SIDE, 2 * kc), BF16), V((2 * rows, qc), BF16),
            V((nx - 1, half, CORES * rows, width // TILES), BF16), V((nx - 1, half, CORES * rows, width // TILES), BF16),
            V((nx - 1, half, CORES * rows, width // TILES), BF16), V((nx - 1, half, CORES * rows, width // TILES), BF16),
            V((nx - 1, TILES, rows, width // TILES), BF16), V((TILES, 2 * rows, width // TILES), BF16),
            V((TILES, rows, width // TILES), BF16), V((2, width), F32), pltpu.SMEM(sink.shape, F32),
            dma((12,)), dma, dma((2,)), dma, dma((2,)),
            dma((nx - 1,)), dma((nx - 1, len(steps))), dma((nx - 1,)), dma((nx - 1, len(steps))), dma, dma,
            dma((2, hops)), dma((2, hops, 2)), dma((max(ny - 1, 1), 2)), dma((max(ny - 1, 1), 2)),
            dma, dma((2,)), dma, dma((nx - 1, 3, half)), dma, dma((nx - 1, 2, TILES)), dma, dma,
        ],
        compiler_params=pltpu.CompilerParams(
            collective_id=0, has_side_effects=True, vmem_limit_bytes=60 * 1024 * 1024
        ),
    )(
        lat, ctx, cond, ctx_cond,
        w_shift, w_scale, w_gate, w_q, w_k, w_v, w_o, sink,
    )


def solution(mesh):
    in_specs = (
        P(("sp", "tp"), None), P("sp", None), P(), P(), P("sp", "tp"), P("sp", "tp"), P("sp", "tp"),
        P(None, "tp"), P(None, "tp"), P(None, "tp"), P("tp", None), P(),
    )
    return jax.shard_map(
        shards, mesh=mesh, in_specs=in_specs, out_specs=P(("sp", "tp"), None), check_vma=False
    )
```
